32 devices in a mesh: sp: 8 (over z, x), tp: 4 (over y, core).
Axes of the slice: x: 2, y: 2, z: 4, core: 2. Of those that a mesh axis runs over, the one named last changes fastest.
Arguments:
- residual: bfloat16 [2048, 2048], P('sp', 'tp'), may hold values from -48 to 48
- queries: bfloat16 [2048, 1024], P('sp', 'tp'), may hold values from -6 to 6
- key_rows: bfloat16 [2048, 512], P('sp', 'tp'), may hold values from -6 to 6
- value_rows: bfloat16 [2048, 512], P('sp', 'tp'), may hold values from -6 to 6
- break_shift: bfloat16 [4, 2048], P('tp', 'sp'), may hold values from -20 to 0
- head_gain: float32 [1024], P('tp'), may hold values from 0.1 to 1.9
- out_weight: bfloat16 [1024, 2048], P('tp'), may hold values from -0.1875 to 0.1875
- mlp_gain: float32 [2048], replicated, may hold values from 0.1 to 1.9
- up_weight: bfloat16 [2048, 8192], P('sp', 'tp'), may hold values from -0.125 to 0.125
- down_weight: bfloat16 [8192, 2048], P('tp', 'sp'), may hold values from -0.0625 to 0.0625
Outputs:
- layer_out: bfloat16 [2048, 2048], P('sp', 'tp')
The draws below stay inside these ranges and needn't reach their ends.
All inputs are finite; a program needn't handle non-finite values.
Results may differ from the reference program's by a relative error of at most 0.013.
Values may be sent and summed in bfloat16 or wider, within the bound.
A program may use at most 128 MiB of HBM per device.

```python
import math
import jax
import jax.numpy as jnp
from jax import lax

D = 2048
HEADS = 8
KEY_VALUE_HEADS = 4
HEAD_DIM = 128
FF = 8192
TOK_DEV = 256
TOKEN_POSITIONS = 2048
KEY_BLOCK = 2048


def draw_residual(key, part):
    noise_key, row_key = jax.random.split(jax.random.fold_in(key, 11), 2)
    column_scale = jnp.exp(math.log(3.0) * jnp.arange(D, dtype=jnp.float32) / D)
    entries = jax.random.truncated_normal(noise_key, -6.0, 6.0, (TOKEN_POSITIONS, D), jnp.float32)
    row_scale = jnp.exp(jax.random.uniform(row_key, (TOKEN_POSITIONS, 1), jnp.float32, 0.0, math.log(10.0)))
    return (entries * row_scale * column_scale / 4.0).astype(jnp.bfloat16)


def draw_break_shift(key, part):
    variety_random_key, frequency_random_key, quick_random_key, block_random_key, spike_random_key, depth_random_key = jax.random.split(jax.random.fold_in(key, 29), 6)
    ranking = jax.random.permutation(variety_random_key, KEY_VALUE_HEADS)
    slow_heads = (ranking < KEY_VALUE_HEADS // 2).astype(jnp.float32)[:, None]
    slow_level = -math.log(float(TOKEN_POSITIONS)) + jax.random.uniform(frequency_random_key, (KEY_VALUE_HEADS, 1), jnp.float32, math.log(0.5), 0.0)
    fast_level = jax.random.uniform(quick_random_key, (KEY_VALUE_HEADS, 1), jnp.float32, -4.5, -3.5)
    baseline_level = slow_heads * slow_level + (1.0 - slow_heads) * fast_level
    block_raise = jax.random.uniform(block_random_key, (KEY_VALUE_HEADS, TOKEN_POSITIONS // TOK_DEV), jnp.float32, 0.0, math.log(4.0))
    block_raise = jnp.repeat(block_raise, TOK_DEV, axis=1)
    spike_locations = jax.random.randint(spike_random_key, (3,), 0, TOKEN_POSITIONS)
    spike_flag = jnp.any(jnp.arange(TOKEN_POSITIONS, dtype=jnp.int32)[None, :] == spike_locations[:, None], axis=0)
    spike_level = jax.random.uniform(depth_random_key, (KEY_VALUE_HEADS, TOKEN_POSITIONS), jnp.float32, -1.6, -0.6)
    return jnp.where(spike_flag[None, :], spike_level, baseline_level + block_raise).astype(jnp.bfloat16)


def block_levels(own_key, dims, shards, smallest, high):
    loudness, own = 1.0, jax.random.fold_in(own_key, 6)
    for dim, blocks in shards:
        steps = jnp.exp(jax.random.uniform(jax.random.fold_in(own, dim), (blocks,), jnp.float32, smallest / len(shards), high / len(shards)))
        loudness = loudness * jnp.repeat(steps, dims[dim] // blocks).reshape([-1 if axis == dim else 1 for axis in range(len(dims))])
    return loudness


def noise(stream_key, dims, deviation, bound, pieces=(), kind=jnp.bfloat16):
    values = deviation * jax.random.normal(stream_key, dims, jnp.float32)
    if pieces:
        values = values * block_levels(stream_key, dims, pieces, -0.22, 0.18)
    return jnp.clip(values, -bound, bound).astype(kind)


def setup_inputs(seed: int = 0) -> dict:
    key_of = jax.random.split(jax.random.key(seed), 11)
    return {
        "residual": draw_residual(jax.random.fold_in(key_of[10], 71), 0),
        "queries": noise(key_of[1], (TOKEN_POSITIONS, HEADS * HEAD_DIM), 1.0, 6.0, ((0, 8), (1, 4))),
        "key_rows": noise(key_of[2], (TOKEN_POSITIONS, KEY_VALUE_HEADS * HEAD_DIM), 1.0, 6.0, ((0, 8), (1, 4))),
        "value_rows": noise(key_of[3], (TOKEN_POSITIONS, KEY_VALUE_HEADS * HEAD_DIM), 1.0, 6.0, ((0, 8), (1, 4))),
        "break_shift": draw_break_shift(jax.random.fold_in(key_of[10], 71), 0),
        "head_gain": jnp.clip(1.0 + 0.18 * jax.random.normal(key_of[5], (HEADS * HEAD_DIM,), jnp.float32), 0.1, 1.9),
        "out_weight": noise(key_of[6], (HEADS * HEAD_DIM, D), (HEADS * HEAD_DIM) ** -0.5, 0.1875, ((0, 4),)),
        "mlp_gain": jnp.clip(1.0 + 0.18 * jax.random.normal(key_of[7], (D,), jnp.float32), 0.1, 1.9),
        "up_weight": noise(key_of[8], (D, FF), D ** -0.5, 0.125, ((0, 8), (1, 4))),
        "down_weight": noise(key_of[9], (FF, D), FF ** -0.5, 0.0625, ((0, 4), (1, 8))),
    }


eps = 1e-06

def reference(residual, queries, key_rows, value_rows, break_shift, head_gain, out_weight, mlp_gain, up_weight, down_weight):
    group_size = HEADS // KEY_VALUE_HEADS
    block_total = TOKEN_POSITIONS // KEY_BLOCK
    score_scale = HEAD_DIM ** (-0.5)
    query_grid = queries.astype(jnp.float32).reshape(TOKEN_POSITIONS, KEY_VALUE_HEADS, group_size, HEAD_DIM)
    key_grid = key_rows.astype(jnp.float32).reshape(TOKEN_POSITIONS, KEY_VALUE_HEADS, HEAD_DIM)
    value_grid = value_rows.astype(jnp.float32).reshape(TOKEN_POSITIONS, KEY_VALUE_HEADS, HEAD_DIM)
    shift_grid = break_shift.astype(jnp.float32)

    def query_span(span_index):
        first_pos = span_index * KEY_BLOCK
        query_block = lax.dynamic_slice_in_dim(query_grid, first_pos, KEY_BLOCK, 0)
        query_pos = first_pos + lax.iota(jnp.int32, KEY_BLOCK)

        def one_block(turn_index, state_pair):
            running, broken_after = state_pair
            offset = (span_index - turn_index) * KEY_BLOCK
            key_block_rows = lax.dynamic_slice_in_dim(key_grid, offset, KEY_BLOCK, 0)
            value_block_rows = lax.dynamic_slice_in_dim(value_grid, offset, KEY_BLOCK, 0)
            shift_block = lax.dynamic_slice_in_dim(shift_grid, offset, KEY_BLOCK, 1)
            scores = jnp.einsum('qgjd,kgd->gjqk', query_block, key_block_rows) * score_scale + shift_block[:, None, None, :]
            key_pos = offset + lax.iota(jnp.int32, KEY_BLOCK)
            visible = key_pos[None, None, None, :] < query_pos[None, None, :, None]
            broken = jnp.where(visible, jax.nn.log_sigmoid(-scores), 0.0)
            later = lax.cumsum(broken, axis=3, reverse=True) - broken + broken_after[:, :, :, None]
            weights = jnp.where(visible, jnp.exp(jax.nn.log_sigmoid(scores) + later), 0.0).astype(jnp.bfloat16)
            weights = lax.optimization_barrier(weights).astype(jnp.float32)
            running = running + jnp.einsum('gjqk,kgd->gjqd', weights, value_block_rows)
            return (running, broken_after + lax.optimization_barrier(jnp.sum(broken, axis=3)))
        start_pair = (jnp.zeros((KEY_VALUE_HEADS, group_size, KEY_BLOCK, HEAD_DIM), jnp.float32), jnp.zeros((KEY_VALUE_HEADS, group_size, KEY_BLOCK), jnp.float32))
        running, broken_after = lax.fori_loop(0, span_index + 1, one_block, start_pair)
        return running.transpose(2, 0, 1, 3).reshape(KEY_BLOCK, HEADS, HEAD_DIM)
    mixed = lax.map(query_span, jnp.arange(block_total, dtype=jnp.int32)).reshape(TOKEN_POSITIONS, HEADS, HEAD_DIM)
    power = lax.optimization_barrier(jnp.mean(mixed * mixed, axis=2, keepdims=True))
    attended = (mixed * lax.rsqrt(power + eps) * head_gain.astype(jnp.float32).reshape(HEADS, HEAD_DIM)).astype(jnp.bfloat16)
    attended = attended.reshape(TOKEN_POSITIONS, HEADS * HEAD_DIM)
    hidden_state = (residual.astype(jnp.float32) + jnp.dot(attended, out_weight, preferred_element_type=jnp.float32)).astype(jnp.bfloat16)
    widened = hidden_state.astype(jnp.float32)
    mlp_in = (widened * lax.rsqrt(lax.optimization_barrier(jnp.mean(widened * widened, axis=1, keepdims=True)) + eps) * mlp_gain.astype(jnp.float32)).astype(jnp.bfloat16)
    activated = jnp.square(jax.nn.relu(jnp.dot(mlp_in, up_weight, preferred_element_type=jnp.float32))).astype(jnp.bfloat16)
    return (widened + jnp.dot(activated, down_weight, preferred_element_type=jnp.float32)).astype(jnp.bfloat16)
```

```python
import functools

import jax
import jax.numpy as jnp
from jax import lax
from jax.experimental import pallas as pl
from jax.experimental.pallas import tpu as pltpu
from jax.sharding import PartitionSpec as P

HEAD_DIM = 128


eps = 1e-06


def stick_attention(queries, key_all, value_all, shift_all, first_pos, key_block):
    token_count = queries.shape[0]
    kv_local = key_all.shape[1] // HEAD_DIM
    query_local = queries.shape[1] // HEAD_DIM
    group_size = query_local // kv_local
    stacked = queries.reshape(token_count, kv_local, group_size, HEAD_DIM).transpose(1, 2, 0, 3)
    stacked = stacked.reshape(kv_local, group_size * token_count, HEAD_DIM)
    query_pos = first_pos + lax.iota(jnp.int32, group_size * token_count) % token_count
    score_scale = HEAD_DIM ** (-0.5)
    block_count = (first_pos + token_count - 1 + key_block - 1) // key_block

    def one_block(turn_index, state_pair):
        running, broken_after = state_pair
        offset = (block_count - 1 - turn_index) * key_block
        key_block_rows = lax.dynamic_slice_in_dim(key_all, offset, key_block, 0).reshape(
            key_block, kv_local, HEAD_DIM
        )
        value_block_rows = lax.dynamic_slice_in_dim(value_all, offset, key_block, 0).reshape(
            key_block, kv_local, HEAD_DIM
        )
        shift_block = lax.dynamic_slice_in_dim(shift_all, offset, key_block, 1).astype(jnp.float32)
        scores = jnp.einsum(
            "grd,kgd->grk", stacked, key_block_rows, preferred_element_type=jnp.float32
        )
        scores = scores * score_scale + shift_block[:, None, :]
        key_pos = offset + lax.iota(jnp.int32, key_block)
        visible = key_pos[None, None, :] < query_pos[None, :, None]
        broken = jnp.where(visible, jax.nn.log_sigmoid(-scores), 0.0)
        later = lax.cumsum(broken, axis=2, reverse=True) - broken + broken_after[:, :, None]
        weights = jnp.where(visible, jnp.exp(jax.nn.log_sigmoid(scores) + later), 0.0).astype(
            jnp.bfloat16
        )
        running = running + jnp.einsum(
            "grk,kgd->grd", weights, value_block_rows, preferred_element_type=jnp.float32
        )
        return (running, broken_after + jnp.sum(broken, axis=2))

    start_pair = (
        jnp.zeros((kv_local, group_size * token_count, HEAD_DIM), jnp.float32),
        jnp.zeros((kv_local, group_size * token_count), jnp.float32),
    )
    running, broken_after = lax.fori_loop(0, block_count, one_block, start_pair)
    running = running.reshape(kv_local, group_size, token_count, HEAD_DIM).transpose(2, 0, 1, 3)
    return running.reshape(token_count, query_local, HEAD_DIM)


def gathered_body(
    residual,
    queries,
    key_rows,
    value_rows,
    break_shift,
    head_gain,
    out_weight,
    mlp_gain,
    up_weight,
    down_weight,
):
    token_count = queries.shape[0]
    first_pos = lax.axis_index("sp") * token_count
    key_all, value_all, shift_all = (
        lax.all_gather(key_rows, "sp", axis=0, tiled=True),
        lax.all_gather(value_rows, "sp", axis=0, tiled=True),
        lax.all_gather(break_shift, "sp", axis=1, tiled=True),
    )
    key_block = min(2048, key_all.shape[0])
    mixed = stick_attention(queries, key_all, value_all, shift_all, first_pos, key_block)
    power = jnp.mean(mixed * mixed, axis=2, keepdims=True)
    attended = (mixed * lax.rsqrt(power + eps) * head_gain.reshape(-1, HEAD_DIM)).astype(
        jnp.bfloat16
    )
    attended = attended.reshape(token_count, -1)
    partial_value = jnp.dot(attended, out_weight, preferred_element_type=jnp.float32)
    column_count = residual.shape[1]
    column_start = lax.axis_index("tp") * column_count
    own_part = lax.dynamic_slice_in_dim(
        partial_value, column_start, column_count, 1
    ) + residual.astype(jnp.float32)
    partial_value = lax.dynamic_update_slice_in_dim(partial_value, own_part, column_start, 1)
    hidden_whole = lax.psum(partial_value, "tp").astype(jnp.bfloat16)
    widened = hidden_whole.astype(jnp.float32)
    inverse = lax.rsqrt(jnp.mean(widened * widened, axis=1, keepdims=True) + eps)
    mlp_in = (widened * inverse * mlp_gain).astype(jnp.bfloat16)
    hidden_state = lax.dynamic_slice_in_dim(hidden_whole, column_start, column_count, 1)
    lifted = jnp.dot(
        mlp_in,
        lax.all_gather(up_weight, "sp", axis=0, tiled=True),
        preferred_element_type=jnp.float32,
    )
    activated = jnp.square(jax.nn.relu(lifted)).astype(jnp.bfloat16)
    expanded = jnp.dot(
        activated,
        lax.all_gather(down_weight, "sp", axis=1, tiled=True),
        preferred_element_type=jnp.float32,
    )
    mlp_total = lax.psum_scatter(
        expanded.astype(jnp.bfloat16), "tp", scatter_dimension=1, tiled=True
    ).astype(jnp.float32)
    return (hidden_state.astype(jnp.float32) + mlp_total).astype(jnp.bfloat16)


PAIR = 2
F32, BF16 = jnp.float32, jnp.bfloat16


def sem_bases(depth, members):
    names = (
        ("kvz", depth), ("kvx", depth), ("shz", depth), ("shx", depth),
        ("upz", depth), ("dnz", depth), ("upx", depth), ("dnx", depth),
        ("res", members), ("hid", members), ("pc", PAIR), ("py", 1),
        ("mz", depth), ("my", depth), ("mc", PAIR * depth),
        ("rc", PAIR * depth), ("ry", depth), ("rz", depth),
    )
    base, total = {}, 0
    for name, count in names:
        base[name] = total
        total += count
    return base, total


def layer_kernel(
    depth, members, queries, keys, values, shift, gain, residual, out_weight, mlp_gain, up, down,
    out, kv_all, shift_all, up_all, down_all, own_f32, own_cut, pair_part, y_cut, y_part,
    res_all, hid_cut, hid_all, rows_all, share, pair_share, y_sum, y_share, z_sum, z_share,
    own_total, send_sem, recv_sem, local_sem,
):
    base, _ = sem_bases(depth, members)
    me, m = lax.axis_index("sp"), lax.axis_index("tp")
    z, x, y, c = me // PAIR, me % PAIR, m // PAIR, m % PAIR
    tokens = queries.shape[0]
    row_part = tokens // members
    sub = up_all.shape[1]
    block = up.shape[0]
    column_part = residual.shape[1]

    def toward(e):
        far = z
        bit = 1
        while bit < depth:
            if e & bit:
                far = far + bit - 2 * bit * ((z // bit) % 2)
            bit *= 2
        return far

    def remote(src, dst, name, send, recv, sp=me, tp=m):
        return pltpu.make_async_remote_copy(
            src_ref=src, dst_ref=dst, send_sem=send_sem.at[base[name] + send],
            recv_sem=recv_sem.at[base[name] + recv], device_id={"sp": sp, "tp": tp},
            device_id_type=pl.DeviceIdType.MESH,
        )

    far_x, far_y, far_c = z * PAIR + 1 - x, (1 - y) * PAIR + c, y * PAIR + 1 - c

    barrier = pltpu.get_barrier_semaphore()
    peers = [(toward(e) * PAIR + x, m) for e in range(1, depth)] + [(far_x, m)]
    peers += [(me, (m + d) % members) for d in range(1, members)]
    for sp, tp in peers:
        pl.semaphore_signal(
            barrier, inc=1, device_id={"sp": sp, "tp": tp}, device_id_type=pl.DeviceIdType.MESH
        )
    first = [
        pltpu.make_async_copy(keys, kv_all.at[me, 0], local_sem.at[0]),
        pltpu.make_async_copy(values, kv_all.at[me, 1], local_sem.at[1]),
        pltpu.make_async_copy(shift, shift_all.at[me], local_sem.at[2]),
    ]

    def up_piece(at):
        return up.at[:, pl.ds(pl.multiple_of(at * sub, sub), sub)]

    def down_piece(at):
        return down.at[pl.ds(pl.multiple_of(at * sub, sub), sub), :]

    def up_slot(at):
        return up_all.at[pl.ds(pl.multiple_of(at * block, block), block), :]

    def down_slot(zz, xx):
        return down_all.at[zz, :, pl.ds(pl.multiple_of(xx * block, block), block)]

    own_weights = [
        pltpu.make_async_copy(up_piece(z), up_slot(me), local_sem.at[3]),
        pltpu.make_async_copy(down_piece(z), down_slot(z, x), local_sem.at[4]),
    ]
    for copy in first + own_weights:
        copy.start()
    for copy in first:
        copy.wait()
    pl.semaphore_wait(barrier, len(peers))

    def kv_z(far):
        sp = far * PAIR + x
        return (
            remote(kv_all.at[me], kv_all.at[me], "kvz", far, z, sp=sp),
            remote(shift_all.at[me], shift_all.at[me], "shz", far, z, sp=sp),
        )

    def kv_x(zz, xx):
        at = zz * PAIR + xx
        return (
            remote(kv_all.at[at], kv_all.at[at], "kvx", zz, zz, sp=far_x),
            remote(shift_all.at[at], shift_all.at[at], "shx", zz, zz, sp=far_x),
        )

    def kv_z_in(zz):
        at = zz * PAIR + x
        return (
            remote(kv_all.at[at], kv_all.at[at], "kvz", zz, zz, sp=far_x),
            remote(shift_all.at[at], shift_all.at[at], "shz", zz, zz, sp=far_x),
        )

    def weight_z(far):
        sp = far * PAIR + x
        return (
            remote(up_piece(far), up_slot(me), "upz", far, z, sp=sp),
            remote(down_piece(far), down_slot(z, x), "dnz", far, z, sp=sp),
        )

    def weight_x(zz, xx):
        slot = up_slot(zz * PAIR + xx)
        cell = down_slot(zz, xx)
        return (
            remote(slot, slot, "upx", zz, zz, sp=far_x),
            remote(cell, cell, "dnx", zz, zz, sp=far_x),
        )

    def weight_z_in(zz):
        slot = up_slot(zz * PAIR + x)
        cell = down_slot(zz, x)
        return (
            remote(slot, slot, "upz", zz, zz, sp=far_x),
            remote(cell, cell, "dnz", zz, zz, sp=far_x),
        )

    def start(copies):
        for copy in copies:
            copy.start()

    def wait_send(copies):
        for copy in copies:
            copy.wait_send()

    def wait_recv(copies):
        for copy in copies:
            copy.wait_recv()

    def residual_out(far):
        rows = pl.ds(pl.multiple_of(far * row_part, row_part), row_part)
        return remote(residual.at[rows, :], res_all.at[m], "res", far, m, tp=far)

    for d in range(1, depth):
        @pl.when(z + d < depth)
        def _():
            start(kv_z(z + d))
    start(kv_x(z, x))
    for d in range(1, members):
        residual_out((m + d) % members).start()
    for d in range(1, depth):
        @pl.when(z - d >= 0)
        def _():
            start(weight_z(z - d))
    for copy in own_weights:
        copy.wait()
    start(weight_x(z, x))
    for d in range(1, depth):
        @pl.when(z + d < depth)
        def _():
            wait_send(kv_z(z + d))
    for d in range(1, depth):
        @pl.when(z + d < depth)
        def _():
            start(weight_z(z + d))

    group = queries.shape[1] // HEAD_DIM
    stacked = jnp.concatenate(
        [queries[:, g * HEAD_DIM : (g + 1) * HEAD_DIM] for g in range(group)], axis=0
    )
    grid = (group * tokens, tokens)
    lag = lax.broadcasted_iota(jnp.int32, grid, 1) - lax.broadcasted_iota(
        jnp.int32, grid, 0
    ) % tokens
    square = (tokens, tokens)
    later_keys = jnp.where(
        lax.broadcasted_iota(jnp.int32, square, 0) > lax.broadcasted_iota(jnp.int32, square, 1),
        1.0, 0.0,
    ).astype(BF16)

    def key_step(at, state):
        running, after = state
        scores = lax.dot_general(
            stacked, kv_all[at, 0], (((1,), (1,)), ((), ())), preferred_element_type=F32
        ) * (HEAD_DIM ** (-0.5)) + shift_all[at][0:1, :]
        visible = lag < (me - at) * tokens
        tail = jnp.log(1.0 + jnp.exp(-jnp.abs(scores)))
        broken = jnp.where(visible, -(jnp.maximum(scores, 0.0) + tail), 0.0)
        high = broken.astype(BF16)
        low = (broken - high.astype(F32)).astype(BF16)
        later = jnp.dot(high, later_keys, preferred_element_type=F32) + jnp.dot(
            low, later_keys, preferred_element_type=F32
        )
        stick = jnp.where(
            visible, jnp.exp(jnp.minimum(scores, 0.0) - tail + (later + after)), 0.0
        ).astype(BF16)
        running = running + jnp.dot(stick, kv_all[at, 1], preferred_element_type=F32)
        return running, after + jnp.sum(broken, axis=1, keepdims=True)

    def key_round(r, state):
        zz = z - r

        @pl.when(r > 0)
        def _():
            wait_recv(kv_z_in(zz))
            start(kv_x(zz, x))

        wait_recv(kv_x(zz, 1 - x))
        state = key_step(zz * PAIR + 1, state)
        return key_step(zz * PAIR, state)

    running, _ = lax.fori_loop(
        0, z + 1, key_round,
        (jnp.zeros((group * tokens, HEAD_DIM), F32), jnp.zeros((group * tokens, 1), F32)),
    )
    scaled = running * lax.rsqrt(jnp.mean(running * running, axis=1, keepdims=True) + eps)
    attended = jnp.concatenate(
        [
            scaled[g * tokens : (g + 1) * tokens] * gain[:, g * HEAD_DIM : (g + 1) * HEAD_DIM]
            for g in range(group)
        ],
        axis=1,
    ).astype(BF16)
    for mm in range(members):
        product = jnp.dot(
            attended[mm * row_part : (mm + 1) * row_part], out_weight[...],
            preferred_element_type=F32,
        )
        own_f32[mm] = product
        own_cut[mm] = product.astype(BF16)

    def pair_out(yy):
        return remote(own_cut.at[yy * PAIR + 1 - c], pair_part.at[yy], "pc", yy, yy, tp=far_c)

    for yy in range(PAIR):
        pair_out(yy).start()

    def weight_forward(e):
        wait_recv(weight_z_in(toward(e)))
        start(weight_x(toward(e), x))

    for yy in range(PAIR):
        pair_out(yy).wait_recv()
    y_cut[...] = (own_f32[far_y] + pair_part[1 - y].astype(F32)).astype(BF16)
    y_out = remote(y_cut, y_part, "py", 0, 0, tp=far_y)
    y_out.start()
    res_all[m] = residual[pl.ds(pl.multiple_of(m * row_part, row_part), row_part), :]
    for d in range(1, members):
        far = (m + d) % members
        remote(res_all.at[far], res_all.at[far], "res", far, far, tp=far).wait_recv()
    y_out.wait_recv()
    hidden = jnp.concatenate([res_all[mm].astype(F32) for mm in range(members)], axis=1)
    hidden = hidden + (own_f32[m] + pair_part[y].astype(F32) + y_part[...].astype(F32))
    hidden = hidden.astype(BF16)
    for mm in range(members):
        hid_cut[mm] = hidden[:, mm * column_part : (mm + 1) * column_part]
    widened = hidden.astype(F32)
    inverse = lax.rsqrt(jnp.mean(widened * widened, axis=1, keepdims=True) + eps)
    rows_all[z, m] = (widened * inverse * mlp_gain[...]).astype(BF16)

    def rows_z(far):
        return remote(rows_all.at[z, m], rows_all.at[z, m], "mz", far, z, sp=far * PAIR + x)

    def rows_z_in(zz):
        return remote(rows_all.at[zz, m], rows_all.at[zz, m], "mz", zz, zz, sp=far_x)

    def rows_y(zz, mm):
        return remote(rows_all.at[zz, mm], rows_all.at[zz, mm], "my", zz, zz, tp=far_y)

    def rows_c(zz, yy, cc):
        cell = rows_all.at[zz, yy * PAIR + cc]
        return remote(cell, cell, "mc", zz * PAIR + yy, zz * PAIR + yy, tp=far_c)

    def hid_out(far):
        return remote(hid_cut.at[far], hid_all.at[m], "hid", far, m, tp=far)

    for e in range(1, depth):
        rows_z(toward(e)).start()
    rows_y(z, m).start()
    rows_c(z, y, c).start()
    for d in range(1, members):
        hid_out((m + d) % members).start()
    hid_all[m] = hid_cut[m]
    for e in range(1, depth):
        weight_forward(e)
        far = toward(e)
        rows_z_in(far).wait_recv()
        rows_y(far, m).start()
        rows_c(far, y, c).start()
    for e in range(depth):
        far = toward(e)
        rows_y(far, far_y).wait_recv()
        rows_c(far, 1 - y, c).start()

    for e in range(depth):
        wait_recv(weight_x(toward(e), 1 - x))

    def share_c(zz, yy):
        return remote(
            share.at[zz, yy * PAIR + 1 - c], pair_share.at[zz, yy], "rc",
            zz * PAIR + yy, zz * PAIR + yy, tp=far_c,
        )

    def share_y(zz):
        return remote(y_sum.at[zz], y_share.at[zz], "ry", zz, zz, tp=far_y)

    def share_z(far):
        return remote(z_sum.at[far], z_share.at[z], "rz", far, z, sp=far * PAIR + x)

    def share_z_in(zz):
        return remote(z_sum.at[zz], z_share.at[zz], "rz", zz, zz, sp=far_x)

    def feed(k, carry):
        zz = (z + 1 + k) % depth
        for yy in range(PAIR):
            rows_c(zz, yy, 1 - c).wait_recv()
        rows = rows_all[zz].reshape(tokens, rows_all.shape[3])
        lifted = jnp.dot(rows, up_all[...], preferred_element_type=F32)
        activated = jnp.square(jnp.maximum(lifted, 0.0)).astype(BF16)
        for mm in range(members):
            share[zz, mm] = jnp.dot(
                activated, down_all[mm], preferred_element_type=F32
            ).astype(BF16)
        for yy in range(PAIR):
            share_c(zz, yy).start()
        return carry

    lax.fori_loop(0, depth, feed, 0)

    def fold_pair(k, carry):
        zz = (z + 1 + k) % depth
        for yy in range(PAIR):
            share_c(zz, yy).wait_recv()
        y_sum[zz] = (
            share[zz, far_y].astype(F32) + pair_share[zz, 1 - y].astype(F32)
        ).astype(BF16)
        share_y(zz).start()
        return carry

    lax.fori_loop(0, depth, fold_pair, 0)

    def fold_y(k, carry):
        zz = (z + 1 + k) % depth
        share_y(zz).wait_recv()
        total = (
            share[zz, m].astype(F32) + pair_share[zz, y].astype(F32) + y_share[zz].astype(F32)
        )

        @pl.when(k < depth - 1)
        def _():
            z_sum[zz] = total.astype(BF16)
            share_z(zz).start()

        @pl.when(k == depth - 1)
        def _():
            own_total[...] = total

        return carry

    lax.fori_loop(0, depth, fold_y, 0)
    for d in range(1, members):
        far = (m + d) % members
        remote(hid_all.at[far], hid_all.at[far], "hid", far, far, tp=far).wait_recv()
    total = own_total[...]
    for e in range(1, depth):
        share_z_in(toward(e)).wait_recv()
        total = total + z_share[toward(e)].astype(F32)
    total = total + hid_all[...].astype(F32).reshape(tokens, column_part)
    out[...] = total.astype(BF16)

    def kv_sent(r, carry):
        wait_send(kv_x(z - r, x))
        return carry

    lax.fori_loop(0, z + 1, kv_sent, 0)
    for yy in range(PAIR):
        pair_out(yy).wait_send()
    y_out.wait_send()
    for d in range(1, members):
        residual_out((m + d) % members).wait_send()
        hid_out((m + d) % members).wait_send()
    for e in range(depth):
        far = toward(e)
        wait_send(weight_x(far, x))
        rows_y(far, m).wait_send()
        rows_c(far, y, c).wait_send()
        rows_c(far, 1 - y, c).wait_send()
        for yy in range(PAIR):
            share_c(far, yy).wait_send()
        share_y(far).wait_send()
        if e:
            wait_send(weight_z(far))
            rows_z(far).wait_send()
            share_z(far).wait_send()


def whole_layer(depth, members, args):
    (residual, queries, key_rows, value_rows, break_shift, head_gain, out_weight, mlp_gain,
     up_weight, down_weight) = args
    tokens, width = residual.shape[0], out_weight.shape[1]
    positions = depth * PAIR
    sub = up_weight.shape[1] // depth
    column_part = residual.shape[1]
    row_part = tokens // members
    shift = jnp.broadcast_to(break_shift.astype(F32), (8, tokens))
    _, sems = sem_bases(depth, members)
    vmem = pl.BlockSpec(memory_space=pltpu.VMEM)
    anywhere = pl.BlockSpec(memory_space=pl.ANY)
    return pl.pallas_call(
        functools.partial(layer_kernel, depth, members),
        out_shape=jax.ShapeDtypeStruct(residual.shape, BF16),
        in_specs=[vmem, anywhere, anywhere, anywhere, vmem, vmem, vmem, vmem, anywhere, anywhere],
        out_specs=vmem,
        scratch_shapes=[
            pltpu.VMEM((positions, 2, tokens, HEAD_DIM), BF16),
            pltpu.VMEM((positions, 8, tokens), F32),
            pltpu.VMEM((width, sub), BF16),
            pltpu.VMEM((depth, sub, column_part), BF16),
            pltpu.VMEM((members, row_part, width), F32),
            pltpu.VMEM((members, row_part, width), BF16),
            pltpu.VMEM((PAIR, row_part, width), BF16),
            pltpu.VMEM((row_part, width), BF16),
            pltpu.VMEM((row_part, width), BF16),
            pltpu.VMEM((members, row_part, column_part), BF16),
            pltpu.VMEM((members, row_part, column_part), BF16),
            pltpu.VMEM((members, row_part, column_part), BF16),
            pltpu.VMEM((depth, members, row_part, width), BF16),
            pltpu.VMEM((depth, members, tokens, column_part), BF16),
            pltpu.VMEM((depth, PAIR, tokens, column_part), BF16),
            pltpu.VMEM((depth, tokens, column_part), BF16),
            pltpu.VMEM((depth, tokens, column_part), BF16),
            pltpu.VMEM((depth, tokens, column_part), BF16),
            pltpu.VMEM((depth, tokens, column_part), BF16),
            pltpu.VMEM((tokens, column_part), F32),
            pltpu.SemaphoreType.DMA((sems,)),
            pltpu.SemaphoreType.DMA((sems,)),
            pltpu.SemaphoreType.DMA((5,)),
        ],
        compiler_params=pltpu.CompilerParams(
            collective_id=0, has_side_effects=True, vmem_limit_bytes=60 * 1024 * 1024
        ),
        name="layer",
    )(
        queries, key_rows, value_rows, shift, head_gain[None, :], residual, out_weight,
        mlp_gain[None, :], up_weight, down_weight,
    )


def fits(depth, members, residual, key_rows, up_weight, down_weight):
    return (
        depth == members == PAIR * PAIR
        and key_rows.shape[1] == HEAD_DIM
        and residual.shape[0] % (128 * PAIR) == 0
        and up_weight.shape[0] % 128 == 0
        and down_weight.shape[1] * PAIR == residual.shape[1]
        and up_weight.shape[0] == down_weight.shape[1]
        and up_weight.shape[1] % (128 * depth) == 0
    )


def body(positions, members, *args):
    depth = positions // PAIR
    if fits(depth, members, args[0], args[2], args[8], args[9]):
        return whole_layer(depth, members, args)
    return gathered_body(*args)


def solution(mesh):
    in_specs = (
        P("sp", "tp"),
        P("sp", "tp"),
        P("sp", "tp"),
        P("sp", "tp"),
        P("tp", "sp"),
        P("tp"),
        P("tp", None),
        P(),
        P("sp", "tp"),
        P("tp", "sp"),
    )
    out_specs = P("sp", "tp")
    return jax.shard_map(
        functools.partial(body, mesh.shape["sp"], mesh.shape["tp"]), mesh=mesh, in_specs=in_specs, out_specs=out_specs, check_vma=False)
```

```python
import functools

import jax
import jax.numpy as jnp
from jax import lax
from jax.experimental import pallas as pl
from jax.experimental.pallas import tpu as pltpu
from jax.sharding import PartitionSpec as P

HEAD_DIM = 128


eps = 1e-06


def stick_attention(queries, key_all, value_all, shift_all, first_pos, key_block):
    token_count = queries.shape[0]
    kv_local = key_all.shape[1] // HEAD_DIM
    query_local = queries.shape[1] // HEAD_DIM
    group_size = query_local // kv_local
    stacked = queries.reshape(token_count, kv_local, group_size, HEAD_DIM).transpose(1, 2, 0, 3)
    stacked = stacked.reshape(kv_local, group_size * token_count, HEAD_DIM)
    query_pos = first_pos + lax.iota(jnp.int32, group_size * token_count) % token_count
    score_scale = HEAD_DIM ** (-0.5)
    block_count = (first_pos + token_count - 1 + key_block - 1) // key_block

    def one_block(turn_index, state_pair):
        running, broken_after = state_pair
        offset = (block_count - 1 - turn_index) * key_block
        key_block_rows = lax.dynamic_slice_in_dim(key_all, offset, key_block, 0).reshape(
            key_block, kv_local, HEAD_DIM
        )
        value_block_rows = lax.dynamic_slice_in_dim(value_all, offset, key_block, 0).reshape(
            key_block, kv_local, HEAD_DIM
        )
        shift_block = lax.dynamic_slice_in_dim(shift_all, offset, key_block, 1).astype(jnp.float32)
        scores = jnp.einsum(
            "grd,kgd->grk", stacked, key_block_rows, preferred_element_type=jnp.float32
        )
        scores = scores * score_scale + shift_block[:, None, :]
        key_pos = offset + lax.iota(jnp.int32, key_block)
        visible = key_pos[None, None, :] < query_pos[None, :, None]
        broken = jnp.where(visible, jax.nn.log_sigmoid(-scores), 0.0)
        later = lax.cumsum(broken, axis=2, reverse=True) - broken + broken_after[:, :, None]
        weights = jnp.where(visible, jnp.exp(jax.nn.log_sigmoid(scores) + later), 0.0).astype(
            jnp.bfloat16
        )
        running = running + jnp.einsum(
            "grk,kgd->grd", weights, value_block_rows, preferred_element_type=jnp.float32
        )
        return (running, broken_after + jnp.sum(broken, axis=2))

    start_pair = (
        jnp.zeros((kv_local, group_size * token_count, HEAD_DIM), jnp.float32),
        jnp.zeros((kv_local, group_size * token_count), jnp.float32),
    )
    running, broken_after = lax.fori_loop(0, block_count, one_block, start_pair)
    running = running.reshape(kv_local, group_size, token_count, HEAD_DIM).transpose(2, 0, 1, 3)
    return running.reshape(token_count, query_local, HEAD_DIM)


def gathered_body(
    residual,
    queries,
    key_rows,
    value_rows,
    break_shift,
    head_gain,
    out_weight,
    mlp_gain,
    up_weight,
    down_weight,
):
    token_count = queries.shape[0]
    first_pos = lax.axis_index("sp") * token_count
    key_all, value_all, shift_all = (
        lax.all_gather(key_rows, "sp", axis=0, tiled=True),
        lax.all_gather(value_rows, "sp", axis=0, tiled=True),
        lax.all_gather(break_shift, "sp", axis=1, tiled=True),
    )
    key_block = min(2048, key_all.shape[0])
    mixed = stick_attention(queries, key_all, value_all, shift_all, first_pos, key_block)
    power = jnp.mean(mixed * mixed, axis=2, keepdims=True)
    attended = (mixed * lax.rsqrt(power + eps) * head_gain.reshape(-1, HEAD_DIM)).astype(
        jnp.bfloat16
    )
    attended = attended.reshape(token_count, -1)
    partial_value = jnp.dot(attended, out_weight, preferred_element_type=jnp.float32)
    column_count = residual.shape[1]
    column_start = lax.axis_index("tp") * column_count
    own_part = lax.dynamic_slice_in_dim(
        partial_value, column_start, column_count, 1
    ) + residual.astype(jnp.float32)
    partial_value = lax.dynamic_update_slice_in_dim(partial_value, own_part, column_start, 1)
    hidden_whole = lax.psum(partial_value, "tp").astype(jnp.bfloat16)
    widened = hidden_whole.astype(jnp.float32)
    inverse = lax.rsqrt(jnp.mean(widened * widened, axis=1, keepdims=True) + eps)
    mlp_in = (widened * inverse * mlp_gain).astype(jnp.bfloat16)
    hidden_state = lax.dynamic_slice_in_dim(hidden_whole, column_start, column_count, 1)
    lifted = jnp.dot(
        mlp_in,
        lax.all_gather(up_weight, "sp", axis=0, tiled=True),
        preferred_element_type=jnp.float32,
    )
    activated = jnp.square(jax.nn.relu(lifted)).astype(jnp.bfloat16)
    expanded = jnp.dot(
        activated,
        lax.all_gather(down_weight, "sp", axis=1, tiled=True),
        preferred_element_type=jnp.float32,
    )
    mlp_total = lax.psum_scatter(
        expanded.astype(jnp.bfloat16), "tp", scatter_dimension=1, tiled=True
    ).astype(jnp.float32)
    return (hidden_state.astype(jnp.float32) + mlp_total).astype(jnp.bfloat16)


PAIR = 2
F32, BF16 = jnp.float32, jnp.bfloat16


def sem_bases(depth, members):
    names = (
        ("kvz", depth), ("kvx", depth), ("shz", depth), ("shx", depth),
        ("upz", depth), ("dnz", depth), ("upx", depth), ("dnx", depth),
        ("res", members), ("hid", members), ("pc", PAIR), ("py", 1),
        ("mz", PAIR * depth), ("my", depth), ("mc", PAIR * depth),
        ("rc", PAIR * depth), ("ry", depth), ("rz", depth),
    )
    base, total = {}, 0
    for name, count in names:
        base[name] = total
        total += count
    return base, total


def layer_kernel(
    depth, members, queries, keys, values, shift, gain, residual, out_weight, mlp_gain, up, down,
    out, kv_all, shift_all, up_all, down_all, own_f32, own_cut, pair_part, y_cut, y_part,
    res_all, hid_cut, hid_all, rows_all, share, pair_share, y_sum, y_share, z_sum, z_share,
    own_total, activated, send_sem, recv_sem, local_sem,
):
    base, _ = sem_bases(depth, members)
    me, m = lax.axis_index("sp"), lax.axis_index("tp")
    z, x, y, c = me // PAIR, me % PAIR, m // PAIR, m % PAIR
    tokens = queries.shape[0]
    row_part = tokens // members
    sub = up_all.shape[1]
    block = up.shape[0]
    column_part = residual.shape[1]

    def toward(e):
        far = z
        bit = 1
        while bit < depth:
            if e & bit:
                far = far + bit - 2 * bit * ((z // bit) % 2)
            bit *= 2
        return far

    inner = ((z + 1) // 2) % 2
    near = [toward(1), toward(2) + inner * (toward(3) - toward(2))]
    near.append(toward(3) + inner * (toward(2) - toward(3)))

    def remote(src, dst, name, send, recv, sp=me, tp=m):
        return pltpu.make_async_remote_copy(
            src_ref=src, dst_ref=dst, send_sem=send_sem.at[base[name] + send],
            recv_sem=recv_sem.at[base[name] + recv], device_id={"sp": sp, "tp": tp},
            device_id_type=pl.DeviceIdType.MESH,
        )

    far_x, far_y, far_c = z * PAIR + 1 - x, (1 - y) * PAIR + c, y * PAIR + 1 - c

    barrier = pltpu.get_barrier_semaphore()
    peers = [(toward(e) * PAIR + x, m) for e in range(1, depth)] + [(far_x, m)]
    peers += [(me, (m + d) % members) for d in range(1, members)]
    for sp, tp in peers:
        pl.semaphore_signal(
            barrier, inc=1, device_id={"sp": sp, "tp": tp}, device_id_type=pl.DeviceIdType.MESH
        )
    first = [
        pltpu.make_async_copy(keys, kv_all.at[me, 0], local_sem.at[0]),
        pltpu.make_async_copy(values, kv_all.at[me, 1], local_sem.at[1]),
        pltpu.make_async_copy(shift, shift_all.at[me], local_sem.at[2]),
    ]

    def up_piece(at):
        return up.at[:, pl.ds(pl.multiple_of(at * sub, sub), sub)]

    def down_piece(at):
        return down.at[pl.ds(pl.multiple_of(at * sub, sub), sub), :]

    def up_slot(at):
        return up_all.at[pl.ds(pl.multiple_of(at * block, block), block), :]

    def down_slot(zz, xx):
        return down_all.at[zz, :, pl.ds(pl.multiple_of(xx * block, block), block)]

    own_weights = [
        pltpu.make_async_copy(up_piece(z), up_slot(me), local_sem.at[3]),
        pltpu.make_async_copy(down_piece(z), down_slot(z, x), local_sem.at[4]),
    ]
    for copy in first + own_weights:
        copy.start()
    for copy in first:
        copy.wait()
    pl.semaphore_wait(barrier, len(peers))

    def kv_z(far):
        sp = far * PAIR + x
        return (
            remote(kv_all.at[me], kv_all.at[me], "kvz", far, z, sp=sp),
            remote(shift_all.at[me], shift_all.at[me], "shz", far, z, sp=sp),
        )

    def kv_x(zz, xx):
        at = zz * PAIR + xx
        return (
            remote(kv_all.at[at], kv_all.at[at], "kvx", zz, zz, sp=far_x),
            remote(shift_all.at[at], shift_all.at[at], "shx", zz, zz, sp=far_x),
        )

    def kv_z_in(zz):
        at = zz * PAIR + x
        return (
            remote(kv_all.at[at], kv_all.at[at], "kvz", zz, zz, sp=far_x),
            remote(shift_all.at[at], shift_all.at[at], "shz", zz, zz, sp=far_x),
        )

    def weight_z(far):
        sp = far * PAIR + x
        return (
            remote(up_piece(far), up_slot(me), "upz", far, z, sp=sp),
            remote(down_piece(far), down_slot(z, x), "dnz", far, z, sp=sp),
        )

    def weight_x(zz, xx):
        slot = up_slot(zz * PAIR + xx)
        cell = down_slot(zz, xx)
        return (
            remote(slot, slot, "upx", zz, zz, sp=far_x),
            remote(cell, cell, "dnx", zz, zz, sp=far_x),
        )

    def weight_z_in(zz):
        slot = up_slot(zz * PAIR + x)
        cell = down_slot(zz, x)
        return (
            remote(slot, slot, "upz", zz, zz, sp=far_x),
            remote(cell, cell, "dnz", zz, zz, sp=far_x),
        )

    def start(copies):
        for copy in copies:
            copy.start()

    def wait_send(copies):
        for copy in copies:
            copy.wait_send()

    def wait_recv(copies):
        for copy in copies:
            copy.wait_recv()

    def residual_out(far):
        rows = pl.ds(pl.multiple_of(far * row_part, row_part), row_part)
        return remote(residual.at[rows, :], res_all.at[m], "res", far, m, tp=far)

    for d in range(1, depth):
        @pl.when(z + d < depth)
        def _():
            start(kv_z(z + d))
    start(kv_x(z, x))
    for d in range(1, members):
        residual_out((m + d) % members).start()
    for far in near:
        @pl.when(far < z)
        def _():
            start(weight_z(far))
    for copy in own_weights:
        copy.wait()

    @pl.when(z == 0)
    def _():
        start(weight_x(z, x))

    for d in range(1, depth):
        @pl.when(z + d < depth)
        def _():
            wait_send(kv_z(z + d))
    for far in near:
        @pl.when(far > z)
        def _():
            start(weight_z(far))

    group = queries.shape[1] // HEAD_DIM
    stacked = jnp.concatenate(
        [queries[:, g * HEAD_DIM : (g + 1) * HEAD_DIM] for g in range(group)], axis=0
    )
    grid = (group * tokens, tokens)
    lag = lax.broadcasted_iota(jnp.int32, grid, 1) - lax.broadcasted_iota(
        jnp.int32, grid, 0
    ) % tokens
    square = (tokens, tokens)
    later_keys = jnp.where(
        lax.broadcasted_iota(jnp.int32, square, 0) > lax.broadcasted_iota(jnp.int32, square, 1),
        1.0, 0.0,
    ).astype(BF16)

    def key_step(at, state):
        running, after = state
        scores = lax.dot_general(
            stacked, kv_all[at, 0], (((1,), (1,)), ((), ())), preferred_element_type=F32
        ) * (HEAD_DIM ** (-0.5)) + shift_all[at][0:1, :]
        visible = lag < (me - at) * tokens
        tail = jnp.log(1.0 + jnp.exp(-jnp.abs(scores)))
        broken = jnp.where(visible, -(jnp.maximum(scores, 0.0) + tail), 0.0)
        high = broken.astype(BF16)
        low = (broken - high.astype(F32)).astype(BF16)
        later = jnp.dot(high, later_keys, preferred_element_type=F32) + jnp.dot(
            low, later_keys, preferred_element_type=F32
        )
        stick = jnp.where(
            visible, jnp.exp(jnp.minimum(scores, 0.0) - tail + (later + after)), 0.0
        ).astype(BF16)
        running = running + jnp.dot(stick, kv_all[at, 1], preferred_element_type=F32)
        return running, after + jnp.sum(broken, axis=1, keepdims=True)

    def weight_forward(far):
        for arrived, onward in zip(weight_z_in(far), weight_x(far, x)):
            arrived.wait_recv()
            onward.start()

    def key_round(r, state):
        zz = z - r

        @pl.when(r == 3)
        def _():
            weight_forward(near[0])

        @pl.when(r > 0)
        def _():
            wait_recv(kv_z_in(zz))
            start(kv_x(zz, x))

        @pl.when(jnp.logical_and(r > 0, r == jnp.minimum(z, 2)))
        def _():
            start(weight_x(z, x))

        wait_recv(kv_x(zz, 1 - x))
        state = key_step(zz * PAIR + 1, state)
        return key_step(zz * PAIR, state)

    running, _ = lax.fori_loop(
        0, z + 1, key_round,
        (jnp.zeros((group * tokens, HEAD_DIM), F32), jnp.zeros((group * tokens, 1), F32)),
    )
    scaled = running * lax.rsqrt(jnp.mean(running * running, axis=1, keepdims=True) + eps)
    attended = jnp.concatenate(
        [
            scaled[g * tokens : (g + 1) * tokens] * gain[:, g * HEAD_DIM : (g + 1) * HEAD_DIM]
            for g in range(group)
        ],
        axis=1,
    ).astype(BF16)
    for mm in range(members):
        product = jnp.dot(
            attended[mm * row_part : (mm + 1) * row_part], out_weight[...],
            preferred_element_type=F32,
        )
        own_f32[mm] = product
        own_cut[mm] = product.astype(BF16)

    def pair_out(yy):
        return remote(own_cut.at[yy * PAIR + 1 - c], pair_part.at[yy], "pc", yy, yy, tp=far_c)

    for yy in range(PAIR):
        pair_out(yy).start()

    @pl.when(z < 3)
    def _():
        weight_forward(near[0])

    for yy in range(PAIR):
        pair_out(yy).wait_recv()
    y_cut[...] = (own_f32[far_y] + pair_part[1 - y].astype(F32)).astype(BF16)
    y_out = remote(y_cut, y_part, "py", 0, 0, tp=far_y)
    y_out.start()
    res_all[m] = residual[pl.ds(pl.multiple_of(m * row_part, row_part), row_part), :]
    for d in range(1, members):
        far = (m + d) % members
        remote(res_all.at[far], res_all.at[far], "res", far, far, tp=far).wait_recv()
    y_out.wait_recv()
    hidden = jnp.concatenate([res_all[mm].astype(F32) for mm in range(members)], axis=1)
    hidden = hidden + (own_f32[m] + pair_part[y].astype(F32) + y_part[...].astype(F32))
    hidden = hidden.astype(BF16)
    for mm in range(members):
        hid_cut[mm] = hidden[:, mm * column_part : (mm + 1) * column_part]
    widened = hidden.astype(F32)
    inverse = lax.rsqrt(jnp.mean(widened * widened, axis=1, keepdims=True) + eps)
    rows_all[z, m] = (widened * inverse * mlp_gain[...]).astype(BF16)

    def rows_hop(zz, step):
        return remote(
            rows_all.at[zz, m], rows_all.at[zz, m], "mz",
            zz if step > 0 else depth + zz, zz, sp=(z + step) * PAIR + x,
        )

    def inside(zz):
        return jnp.logical_and(zz >= 0, zz < depth)

    def rows_z_in(zz):
        return remote(rows_all.at[zz, m], rows_all.at[zz, m], "mz", zz, zz, sp=far_x)

    def rows_y(zz, mm):
        return remote(rows_all.at[zz, mm], rows_all.at[zz, mm], "my", zz, zz, tp=far_y)

    def rows_c(zz, yy, cc):
        cell = rows_all.at[zz, yy * PAIR + cc]
        return remote(cell, cell, "mc", zz * PAIR + yy, zz * PAIR + yy, tp=far_c)

    def hid_out(far):
        return remote(hid_cut.at[far], hid_all.at[m], "hid", far, m, tp=far)

    for step in (1, -1):
        @pl.when(inside(z + step))
        def _():
            rows_hop(z, step).start()
    rows_y(z, m).start()
    rows_c(z, y, c).start()
    for d in range(1, members):
        hid_out((m + d) % members).start()
    hid_all[m] = hid_cut[m]
    weight_forward(near[1])
    weight_forward(near[2])
    for d in range(1, depth):
        for step in (1, -1):
            far = z - step * d

            @pl.when(inside(far))
            def _():
                rows_z_in(far).wait_recv()

                @pl.when(inside(z + step))
                def _():
                    rows_hop(far, step).start()

                rows_y(far, m).start()
                rows_c(far, y, c).start()
    for e in range(depth):
        far = toward(e)
        rows_y(far, far_y).wait_recv()
        rows_c(far, 1 - y, c).start()

    for e in range(depth):
        weight_x(toward(e), 1 - x)[0].wait_recv()

    def share_c(zz, yy):
        return remote(
            share.at[zz, yy * PAIR + 1 - c], pair_share.at[zz, yy], "rc",
            zz * PAIR + yy, zz * PAIR + yy, tp=far_c,
        )

    def share_y(zz):
        return remote(y_sum.at[zz], y_share.at[zz], "ry", zz, zz, tp=far_y)

    def share_z(far):
        return remote(z_sum.at[far], z_share.at[z], "rz", far, z, sp=far * PAIR + x)

    def share_z_in(zz):
        return remote(z_sum.at[zz], z_share.at[zz], "rz", zz, zz, sp=far_x)

    def lift(k, carry):
        zz = (z + 1 + k) % depth
        for yy in range(PAIR):
            rows_c(zz, yy, 1 - c).wait_recv()
        rows = rows_all[zz].reshape(tokens, rows_all.shape[3])
        lifted = jnp.dot(rows, up_all[...], preferred_element_type=F32)
        activated[zz] = jnp.square(jnp.maximum(lifted, 0.0)).astype(BF16)
        return carry

    lax.fori_loop(0, depth, lift, 0)
    for e in range(depth):
        weight_x(toward(e), 1 - x)[1].wait_recv()

    def feed(k, carry):
        zz = (z + 1 + k) % depth
        for mm in range(members):
            share[zz, mm] = jnp.dot(
                activated[zz], down_all[mm], preferred_element_type=F32
            ).astype(BF16)
        for yy in range(PAIR):
            share_c(zz, yy).start()

        @pl.when(k > 0)
        def _():
            fold_pair(k - 1)

        return carry

    def fold_pair(k):
        zz = (z + 1 + k) % depth
        for yy in range(PAIR):
            share_c(zz, yy).wait_recv()
        y_sum[zz] = (
            share[zz, far_y].astype(F32) + pair_share[zz, 1 - y].astype(F32)
        ).astype(BF16)
        share_y(zz).start()

    lax.fori_loop(0, depth, feed, 0)
    fold_pair(depth - 1)

    def fold_y(k, carry):
        zz = (z + 1 + k) % depth
        share_y(zz).wait_recv()
        total = (
            share[zz, m].astype(F32) + pair_share[zz, y].astype(F32) + y_share[zz].astype(F32)
        )

        @pl.when(k < depth - 1)
        def _():
            z_sum[zz] = total.astype(BF16)
            share_z(zz).start()

        @pl.when(k == depth - 1)
        def _():
            own_total[...] = total

        return carry

    lax.fori_loop(0, depth, fold_y, 0)
    for d in range(1, members):
        far = (m + d) % members
        remote(hid_all.at[far], hid_all.at[far], "hid", far, far, tp=far).wait_recv()
    total = own_total[...]
    for e in range(1, depth):
        share_z_in(toward(e)).wait_recv()
        total = total + z_share[toward(e)].astype(F32)
    total = total + hid_all[...].astype(F32).reshape(tokens, column_part)
    out[...] = total.astype(BF16)

    def kv_sent(r, carry):
        wait_send(kv_x(z - r, x))
        return carry

    lax.fori_loop(0, z + 1, kv_sent, 0)
    for d in range(depth):
        for step in (1, -1) if d else (1,):
            far = z - step * d

            @pl.when(inside(far))
            def _():
                for hop in (step,) if d else (1, -1):
                    @pl.when(inside(z + hop))
                    def _():
                        rows_hop(far, hop).wait_send()

    for yy in range(PAIR):
        pair_out(yy).wait_send()
    y_out.wait_send()
    for d in range(1, members):
        residual_out((m + d) % members).wait_send()
        hid_out((m + d) % members).wait_send()
    for e in range(depth):
        far = toward(e)
        wait_send(weight_x(far, x))
        rows_y(far, m).wait_send()
        rows_c(far, y, c).wait_send()
        rows_c(far, 1 - y, c).wait_send()
        for yy in range(PAIR):
            share_c(far, yy).wait_send()
        share_y(far).wait_send()
        if e:
            wait_send(weight_z(far))
            share_z(far).wait_send()


def whole_layer(depth, members, args):
    (residual, queries, key_rows, value_rows, break_shift, head_gain, out_weight, mlp_gain,
     up_weight, down_weight) = args
    tokens, width = residual.shape[0], out_weight.shape[1]
    positions = depth * PAIR
    sub = up_weight.shape[1] // depth
    column_part = residual.shape[1]
    row_part = tokens // members
    shift = jnp.broadcast_to(break_shift.astype(F32), (8, tokens))
    _, sems = sem_bases(depth, members)
    vmem = pl.BlockSpec(memory_space=pltpu.VMEM)
    anywhere = pl.BlockSpec(memory_space=pl.ANY)
    return pl.pallas_call(
        functools.partial(layer_kernel, depth, members),
        out_shape=jax.ShapeDtypeStruct(residual.shape, BF16),
        in_specs=[vmem, anywhere, anywhere, anywhere, vmem, vmem, vmem, vmem, anywhere, anywhere],
        out_specs=vmem,
        scratch_shapes=[
            pltpu.VMEM((positions, 2, tokens, HEAD_DIM), BF16),
            pltpu.VMEM((positions, 8, tokens), F32),
            pltpu.VMEM((width, sub), BF16),
            pltpu.VMEM((depth, sub, column_part), BF16),
            pltpu.VMEM((members, row_part, width), F32),
            pltpu.VMEM((members, row_part, width), BF16),
            pltpu.VMEM((PAIR, row_part, width), BF16),
            pltpu.VMEM((row_part, width), BF16),
            pltpu.VMEM((row_part, width), BF16),
            pltpu.VMEM((members, row_part, column_part), BF16),
            pltpu.VMEM((members, row_part, column_part), BF16),
            pltpu.VMEM((members, row_part, column_part), BF16),
            pltpu.VMEM((depth, members, row_part, width), BF16),
            pltpu.VMEM((depth, members, tokens, column_part), BF16),
            pltpu.VMEM((depth, PAIR, tokens, column_part), BF16),
            pltpu.VMEM((depth, tokens, column_part), BF16),
            pltpu.VMEM((depth, tokens, column_part), BF16),
            pltpu.VMEM((depth, tokens, column_part), BF16),
            pltpu.VMEM((depth, tokens, column_part), BF16),
            pltpu.VMEM((tokens, column_part), F32),
            pltpu.VMEM((depth, tokens, sub), BF16),
            pltpu.SemaphoreType.DMA((sems,)),
            pltpu.SemaphoreType.DMA((sems,)),
            pltpu.SemaphoreType.DMA((5,)),
        ],
        compiler_params=pltpu.CompilerParams(
            collective_id=0, has_side_effects=True, vmem_limit_bytes=60 * 1024 * 1024
        ),
        name="layer",
    )(
        queries, key_rows, value_rows, shift, head_gain[None, :], residual, out_weight,
        mlp_gain[None, :], up_weight, down_weight,
    )


def fits(depth, members, residual, key_rows, up_weight, down_weight):
    return (
        depth == members == PAIR * PAIR
        and key_rows.shape[1] == HEAD_DIM
        and residual.shape[0] % (128 * PAIR) == 0
        and up_weight.shape[0] % 128 == 0
        and down_weight.shape[1] * PAIR == residual.shape[1]
        and up_weight.shape[0] == down_weight.shape[1]
        and up_weight.shape[1] % (128 * depth) == 0
    )


def body(positions, members, *args):
    depth = positions // PAIR
    if fits(depth, members, args[0], args[2], args[8], args[9]):
        return whole_layer(depth, members, args)
    return gathered_body(*args)


def solution(mesh):
    in_specs = (
        P("sp", "tp"),
        P("sp", "tp"),
        P("sp", "tp"),
        P("sp", "tp"),
        P("tp", "sp"),
        P("tp"),
        P("tp", None),
        P(),
        P("sp", "tp"),
        P("tp", "sp"),
    )
    out_specs = P("sp", "tp")
    return jax.shard_map(
        functools.partial(body, mesh.shape["sp"], mesh.shape["tp"]), mesh=mesh, in_specs=in_specs, out_specs=out_specs, check_vma=False)
```
